32 devices in a mesh: grp: 2 (over y), fs: 4 (over z), tp: 4 (over x, core).
Axes of the slice: x: 2, y: 2, z: 4, core: 2. Of those that a mesh axis runs over, the one named last changes fastest.
Arguments:
- tokens: bfloat16 [4096, 2048], P(('grp', 'fs')), parts along dimension 0, may hold values from -6 to 6
- norm_gain: float32 [2, 2048], replicated, may hold values from 0.1 to 1.9
- norm_shift: float32 [2, 2048], replicated, may hold values from -3 to 3
- gate_first: bfloat16 [2048, 3072], P('fs', 'tp'), may hold values from -0.125 to 0.125
- up_first: bfloat16 [2048, 3072], P('fs', 'tp'), may hold values from -0.125 to 0.125
- down_first: bfloat16 [3072, 2048], P('tp', 'fs'), may hold values from -0.21875 to 0.21875
- gate_second: bfloat16 [2048, 3072], P('fs', 'tp'), may hold values from -0.125 to 0.125
- up_second: bfloat16 [2048, 3072], P('fs', 'tp'), may hold values from -0.125 to 0.125
- down_second: bfloat16 [3072, 2048], P('tp', 'fs'), may hold values from -0.21875 to 0.21875
Outputs:
- encoded: bfloat16 [4096, 2048], P(('grp', 'fs')), parts along dimension 0
The draws below stay inside these ranges and needn't reach their ends.
There are 2 independent parts, one for each index of `grp`. The reference program is written for one: setup_inputs(seed, part) draws one part's arguments, and reference() takes and returns one part's arrays. A program takes and returns all parts, laid end to end along the dimension named above; an argument that names none is the same for every part. Nothing has to cross between parts.
All inputs are finite; a program needn't handle non-finite values.
Results may differ from the reference program's by a relative error of at most 0.012.
Values may be sent and summed in bfloat16 or wider, within the bound.
No kernel may reach another device: no remote copies, remote signals or barrier semaphores. Data moves between devices by JAX's collectives and lax.ppermute only.
A program may use at most 64 MiB of HBM per device.

```python
import jax
import jax.numpy as jnp
from jax import lax

D = 2048
FF = 3072
TOKENS = 2048
N_TP = 4


def block_scale(rng, extent, cuts, smallest, largest):
    def one(dim, blocks):
        steps = jax.random.uniform(jax.random.fold_in(jax.random.fold_in(rng, 6), dim), (blocks,), jnp.float32, smallest / len(cuts), largest / len(cuts))
        return jnp.repeat(jnp.exp(steps), extent[dim] // blocks).reshape((-1,) + (1,) * (len(extent) - dim - 1))

    factor_of = one(*cuts[0])
    for cut in cuts[1:]:
        factor_of = factor_of * one(*cut)
    return factor_of


def bell_draw(own_key, shape, scale, reach, cuts=(), kind=jnp.bfloat16):
    result = jax.random.normal(own_key, shape, jnp.float32) * scale
    if len(cuts) > 0:
        result = block_scale(own_key, shape, cuts, -0.22, 0.18) * result
    return jnp.clip(result, min=-reach, max=reach).astype(kind)


def setup_inputs(seed: int = 0, part: int = 0) -> dict:
    arg_keys = jax.random.split(jax.random.key(seed), 10)
    part_splits = jax.random.split(jax.random.fold_in(arg_keys[9], part), 10)
    tokens = bell_draw(part_splits[0], (TOKENS, D), 1.0, 6.0, ((0, 4),))
    norm_gain = jnp.clip(1.0 + 0.18 * jax.random.normal(arg_keys[1], (2, D), jnp.float32), 0.1, 1.9)
    norm_shift = bell_draw(arg_keys[2], (2, D), 0.5, 3.0, (), jnp.float32)
    gate_first = bell_draw(arg_keys[3], (D, FF), D ** -0.5, 0.125, ((0, 4), (1, 4)))
    up_first = bell_draw(arg_keys[4], (D, FF), D ** -0.5, 0.125, ((0, 4), (1, 4)))
    down_first = bell_draw(arg_keys[5], (FF, D), (FF // 4) ** -0.5, 0.21875, ((0, 4), (1, 4)))
    gate_second = bell_draw(arg_keys[6], (D, FF), D ** -0.5, 0.125, ((0, 4), (1, 4)))
    up_second = bell_draw(arg_keys[7], (D, FF), D ** -0.5, 0.125, ((0, 4), (1, 4)))
    down_second = bell_draw(arg_keys[8], (FF, D), (FF // 4) ** -0.5, 0.21875, ((0, 4), (1, 4)))
    return {"tokens": tokens, "norm_gain": norm_gain, "norm_shift": norm_shift, "gate_first": gate_first, "up_first": up_first, "down_first": down_first, "gate_second": gate_second, "up_second": up_second, "down_second": down_second}


def post_norm(values, gain, shift):
    mean = lax.optimization_barrier(jnp.mean(values, axis=-1, keepdims=True))
    spread = lax.optimization_barrier(jnp.mean(jnp.square(values - mean), axis=-1, keepdims=True))
    normed = (values - mean) * lax.rsqrt(spread + 1e-05)
    return (normed * gain + shift).astype(jnp.bfloat16)

def feed_forward(stream, gate_w, up_w, down_w):
    gate = jnp.dot(stream, gate_w, preferred_element_type=jnp.float32)
    up = jnp.dot(stream, up_w, preferred_element_type=jnp.float32)
    hidden = (jax.nn.silu(gate) * up).astype(jnp.bfloat16)
    width = FF // N_TP
    total = jnp.zeros((stream.shape[0], down_w.shape[1]), jnp.float32)
    for block in range(N_TP):
        partial_value = jnp.dot(hidden[:, block * width:(block + 1) * width], down_w[block * width:(block + 1) * width], preferred_element_type=jnp.float32).astype(jnp.bfloat16)
        partial_value = lax.optimization_barrier(partial_value)
        total = total + partial_value.astype(jnp.float32)
    return total.astype(jnp.bfloat16)

def reference(tokens, norm_gain, norm_shift, gate_first, up_first, down_first, gate_second, up_second, down_second):
    scale = 2.0 ** 0.25
    branch = feed_forward(tokens, gate_first, up_first, down_first)
    middle = post_norm(scale * tokens.astype(jnp.float32) + 0.5 * branch.astype(jnp.float32), norm_gain[0], norm_shift[0])
    branch2 = feed_forward(middle, gate_second, up_second, down_second)
    return post_norm(scale * middle.astype(jnp.float32) + 0.5 * branch2.astype(jnp.float32), norm_gain[1], norm_shift[1])
```

```python
import jax
import jax.numpy as jnp
from jax import lax
from jax.sharding import PartitionSpec as P


def post_norm(values, gain, shift):
    mean = jnp.mean(values, axis=-1, keepdims=True)
    spread = jnp.mean(jnp.square(values - mean), axis=-1, keepdims=True)
    normed = (values - mean) * lax.rsqrt(spread + 1e-05)
    return (normed * gain + shift).astype(jnp.bfloat16)


def product(a, b):
    return jnp.dot(a, b, preferred_element_type=jnp.float32)


def add(a, b):
    return (a.astype(jnp.float32) + b.astype(jnp.float32)).astype(jnp.bfloat16)


def plain_half_step(stream, gate_w, up_w, down_w, gain, shift):
    width = gate_w.shape[1]
    joined = jnp.concatenate(
        (
            lax.all_gather(gate_w, "fs", axis=0, tiled=True),
            lax.all_gather(up_w, "fs", axis=0, tiled=True),
        ),
        axis=1,
    )
    both = product(stream, joined)
    hidden = (jax.nn.silu(both[:, :width]) * both[:, width:]).astype(jnp.bfloat16)
    down_full = lax.all_gather(down_w, "fs", axis=1, tiled=True)
    branch = lax.psum(product(hidden, down_full).astype(jnp.bfloat16), "tp")
    return post_norm(
        2.0**0.25 * stream.astype(jnp.float32) + 0.5 * branch.astype(jnp.float32), gain, shift
    )


def plain(tokens, gains, shifts, *weights):
    middle = plain_half_step(tokens, *weights[:3], gains[0], shifts[0])
    return plain_half_step(middle, *weights[3:], gains[1], shifts[1])


PAIR = [(0, 1), (1, 0), (2, 3), (3, 2)]
MIDDLE = [(1, 2), (2, 1)]
OUTWARD = [(1, 0), (2, 3)]


def swap_core(v):
    return lax.ppermute(v, "tp", [(t, t ^ 1) for t in range(4)])


def swap_x(v):
    return lax.ppermute(v, "tp", [(t, t ^ 2) for t in range(4)])


def swap_y(v):
    return lax.ppermute(v, "grp", [(0, 1), (1, 0)])


def along(v, table):
    return lax.ppermute(v, "fs", table)


def relay(own, is_mid):
    p1 = along(own, PAIR)
    m1 = along(own, MIDDLE)
    m2 = along(p1, MIDDLE)
    p2 = along(m1, OUTWARD)
    p3 = along(m2, OUTWARD)
    return own, p1, jnp.where(is_mid, m1, p2), jnp.where(is_mid, m2, p3)


def in_order(low_first, mine, other, axis=0):
    return jnp.concatenate(
        (jnp.where(low_first, mine, other), jnp.where(low_first, other, mine)), axis=axis
    )


def line(tokens, gains, shifts, *weights):
    g = lax.axis_index("grp")
    f = lax.axis_index("fs")
    t = lax.axis_index("tp")
    c, x = t % 2, t // 2
    is_mid = (f == 1) | (f == 2)
    first_pair = f < 2
    order = (f, f ^ 1, jnp.where(first_pair, 2, 1), jnp.where(first_pair, 3, 0))
    back = (
        jnp.where(first_pair, f, 3),
        jnp.where(first_pair, f ^ 1, 2),
        jnp.where(first_pair, 2, f ^ 2),
        jnp.where(first_pair, 3, f ^ 2 ^ 1),
    )
    rows, model = tokens.shape
    quarter = model // 4

    def arranged(v, positions):
        return jnp.concatenate(
            [lax.dynamic_slice_in_dim(v, p * quarter, quarter, axis=1) for p in positions], axis=1
        )

    def own_pieces(gate_w, up_w, down_w):
        half = gate_w.shape[1] // 2
        gate_up = jnp.concatenate(
            [lax.dynamic_slice_in_dim(w, g * half, half, axis=1) for w in (gate_w, up_w)], axis=1
        )
        return gate_up, lax.dynamic_slice_in_dim(down_w, g * half, half, axis=0)

    def both_groups(mine):
        block = jnp.stack((mine, swap_y(mine)))
        other = swap_core(block)
        return in_order(c == 0, block, other, axis=1).reshape(2 * rows, model)

    def scattered(part):
        part = part.reshape(2, 2, rows // 2, part.shape[-1])
        other = swap_core(lax.dynamic_index_in_dim(part, 1 - c, 1, keepdims=False))
        part = add(lax.dynamic_index_in_dim(part, c, 1, keepdims=False), other)
        part = add(part[0], swap_y(part[1])).reshape(2, rows // 4, -1)
        other = swap_x(lax.dynamic_index_in_dim(part, 1 - x, 0, keepdims=False))
        return add(lax.dynamic_index_in_dim(part, x, 0, keepdims=False), other)

    def half_step(stream, residual, gate_up, down, gain, shift):
        half = down[0].shape[0]
        both = sum(
            product(stream[:, i * quarter : (i + 1) * quarter], gate_up[i]) for i in range(4)
        )
        hidden = (jax.nn.silu(both[:, :half]) * both[:, half:]).astype(jnp.bfloat16)
        parts = [product(hidden, d).astype(jnp.bfloat16) for d in down]
        branch = jnp.concatenate(
            (scattered(jnp.concatenate(parts[:3], axis=1)), scattered(parts[3])), axis=1
        )
        values = 2.0**0.25 * residual.astype(jnp.float32) + 0.5 * branch.astype(jnp.float32)
        return post_norm(values, gain, shift)

    gains, shifts = arranged(gains, order), arranged(shifts, order)
    own = [own_pieces(*weights[:3]), own_pieces(*weights[3:])]
    gate_up1, down1 = [relay(v, is_mid) for v in own[0]]
    gate_up2, down2 = [relay(v, is_mid) for v in own[1]]

    tokens = arranged(tokens, order)
    my_half = lax.dynamic_slice_in_dim(tokens, c * (rows // 2), rows // 2)
    residual = lax.dynamic_slice_in_dim(my_half, x * (rows // 4), rows // 4)
    stream = both_groups(my_half)
    middle = half_step(stream, residual, gate_up1, down1, gains[0], shifts[0])
    stream = both_groups(in_order(x == 0, middle, swap_x(middle)))
    encoded = half_step(stream, middle, gate_up2, down2, gains[1], shifts[1])
    encoded = arranged(encoded, back)
    encoded = in_order(x == 0, encoded, swap_x(encoded))
    return in_order(c == 0, encoded, swap_core(encoded))


def solution(mesh):
    placed = (
        P(("grp", "fs"), None),
        P(),
        P(),
        P("fs", "tp"),
        P("fs", "tp"),
        P("tp", "fs"),
        P("fs", "tp"),
        P("fs", "tp"),
        P("tp", "fs"),
    )
    sizes = tuple(mesh.shape[a] for a in ("grp", "fs", "tp"))
    body = line if sizes == (2, 4, 4) else plain
    return jax.shard_map(
        body, mesh=mesh, in_specs=placed, out_specs=P(("grp", "fs"), None), check_vma=False
    )
```
